512 devices in a mesh: rep: 2 (over z_hi), fs: 32 (over z_lo, y), tp: 8 (over x, core).
Axes of the slice: x: 4, y: 8, z: 8 (z_hi: 2, z_lo: 4; z = z_hi * 4 + z_lo), core: 2. Of those that a mesh axis runs over, the one named last changes fastest.
Arguments:
- x_early: bfloat16 [7168, 2048], P(('rep', 'fs')), may hold values from -6 to 6
- x_late: bfloat16 [7168, 2048], P(('rep', 'fs')), may hold values from -6 to 6
- grad_out: bfloat16 [7168, 2048], P(('rep', 'fs')), may hold values from -16 to 16
- w_gate: bfloat16 [2048, 3072], P('fs', 'tp'), may hold values from -0.125 to 0.125
- w_up: bfloat16 [2048, 3072], P('fs', 'tp'), may hold values from -0.125 to 0.125
- w_down: bfloat16 [3072, 2048], P('tp', 'fs'), may hold values from -0.109375 to 0.109375
- gate_sum: float32 [2048, 3072], P('fs', 'tp'), may hold values from -160 to 160
- up_sum: float32 [2048, 3072], P('fs', 'tp'), may hold values from -160 to 160
- down_sum: float32 [3072, 2048], P('tp', 'fs'), may hold values from -160 to 160
Outputs:
- out_late: bfloat16 [7168, 2048], P(('rep', 'fs'))
- grad_in: bfloat16 [7168, 2048], P(('rep', 'fs'))
- new_gate_sum: float32 [2048, 3072], P('fs', 'tp')
- new_up_sum: float32 [2048, 3072], P('fs', 'tp')
- new_down_sum: float32 [3072, 2048], P('tp', 'fs')
The draws below stay inside these ranges and needn't reach their ends.
All inputs are finite; a program needn't handle non-finite values.
Results may differ from the reference program's by a relative error of at most 0.018.
Values may be sent and summed in bfloat16 or wider, within the bound.
No kernel may reach another device: no remote copies, remote signals or barrier semaphores. Data moves between devices by JAX's collectives and lax.ppermute only.
A program may use at most 64 MiB of HBM per device.

```python
import jax
import jax.numpy as jnp
from jax import lax

D = 2048
FF = 3072
TOKENS = 7168
N_TP = 8


def strengthened(drawn, key, source, target, blocks, factor):
    def block_of(dim):
        return (jnp.arange(drawn.shape[dim]) // (drawn.shape[dim] // blocks)).reshape((-1,) + (1,) * (drawn.ndim - 1 - dim))

    one_side = jax.random.permutation(key, blocks)[block_of(target)]
    second = (block_of(target) + blocks // 2) % blocks
    return jnp.where((block_of(source) == one_side) | (block_of(source) == second), factor * drawn, drawn)


def steps_of(rng, extent, split, low, high):
    level, own = 1.0, jax.random.fold_in(rng, 6)
    for position, shards_of in split:
        heights = jnp.exp(jax.random.uniform(jax.random.fold_in(own, position), (shards_of,), jnp.float32, low / len(split), high / len(split)))
        level = level * jnp.repeat(heights, extent[position] // shards_of).reshape([-1 if axis == position else 1 for axis in range(len(extent))])
    return level


def bell_draw(key, extent, scale, most, cuts=(), kind=jnp.bfloat16):
    drawn = jax.random.normal(key, extent, jnp.float32) * scale
    if len(cuts) > 0:
        drawn = steps_of(key, extent, cuts, -0.22, 0.18) * drawn
    return jnp.clip(drawn, min=-most, max=most).astype(kind)


def bell_draw_with(rng, dims, spread, limit, split, heavy, dtype=jnp.bfloat16):
    array = spread * jax.random.normal(rng, dims, jnp.float32)
    if split:
        array = array * steps_of(rng, dims, split, -0.22, 0.18)
    return jnp.clip(strengthened(array, jax.random.fold_in(rng, 3), *heavy), -limit, limit).astype(dtype)


def setup_inputs(seed: int = 0) -> dict:
    seeds = jax.random.split(jax.random.key(seed), 10)
    return {
        "x_early": bell_draw(seeds[0], (TOKENS, D), 1.0, 6.0, ((0, 64),)),
        "x_late": bell_draw(seeds[1], (TOKENS, D), 1.0, 6.0, ((0, 64),)),
        "grad_out": bell_draw_with(seeds[2], (TOKENS, D), 1.0, 16.0, ((0, 64),), (0, 1, 64, 4.0)),
        "w_gate": bell_draw(seeds[3], (D, FF), D ** -0.5, 0.125, ((0, 32), (1, 8))),
        "w_up": bell_draw(seeds[4], (D, FF), D ** -0.5, 0.125, ((0, 32), (1, 8))),
        "w_down": bell_draw(seeds[5], (FF, D), FF ** -0.5, 0.109375, ((0, 8), (1, 32))),
        "gate_sum": bell_draw(seeds[6], (D, FF), (0.3 * TOKENS ** 0.5), 160.0, ((0, 32), (1, 8)), jnp.float32),
        "up_sum": bell_draw(seeds[7], (D, FF), (0.3 * TOKENS ** 0.5), 160.0, ((0, 32), (1, 8)), jnp.float32),
        "down_sum": bell_draw(seeds[8], (FF, D), (0.3 * TOKENS ** 0.5), 160.0, ((0, 8), (1, 32)), jnp.float32),
    }


epsilon = 1e-06

def prepare(x_rows):
    wide = x_rows.astype(jnp.float32)
    row_scale = lax.rsqrt(lax.optimization_barrier(jnp.mean(wide * wide, axis=-1, keepdims=True)) + epsilon)
    normed = (wide * row_scale).astype(jnp.bfloat16)
    return (wide, row_scale, normed)

def reference(x_early, x_late, grad_out, w_gate, w_up, w_down, gate_sum, up_sum, down_sum):
    late_wide, late_scale, late_normed = prepare(x_late)
    late_gate = jnp.dot(late_normed, w_gate, preferred_element_type=jnp.float32)
    late_upper = jnp.dot(late_normed, w_up, preferred_element_type=jnp.float32)
    late_hidden = (late_gate * jax.nn.sigmoid(late_gate) * late_upper).astype(jnp.bfloat16)
    block = FF // N_TP
    branch = jnp.zeros(x_late.shape, jnp.float32)
    for column in range(N_TP):
        part = jnp.dot(late_hidden[:, column * block:(column + 1) * block], w_down[column * block:(column + 1) * block], preferred_element_type=jnp.float32)
        branch = branch + part.astype(jnp.bfloat16).astype(jnp.float32)
    out_late = (late_wide + 0.5 * branch).astype(jnp.bfloat16)
    early_wide, early_scale, early_normed = prepare(x_early)
    gate_pre = jnp.dot(early_normed, w_gate, preferred_element_type=jnp.float32)
    up_pre = jnp.dot(early_normed, w_up, preferred_element_type=jnp.float32)
    gate_sig = jax.nn.sigmoid(gate_pre)
    hidden = (gate_pre * gate_sig * up_pre).astype(jnp.bfloat16)
    grad_hidden = 0.5 * jnp.dot(grad_out, w_down.T, preferred_element_type=jnp.float32)
    grad_gate_in = (grad_hidden * up_pre * gate_sig * (1.0 + gate_pre * (1.0 - gate_sig))).astype(jnp.bfloat16)
    grad_up_in = (grad_hidden * gate_pre * gate_sig).astype(jnp.bfloat16)
    grad_normed = jnp.dot(grad_gate_in, w_gate.T, preferred_element_type=jnp.float32)
    grad_normed = grad_normed + jnp.dot(grad_up_in, w_up.T, preferred_element_type=jnp.float32)
    unit_rows = early_wide * early_scale
    inner = lax.optimization_barrier(jnp.mean(grad_normed * unit_rows, axis=-1, keepdims=True))
    grad_in = (grad_out.astype(jnp.float32) + early_scale * (grad_normed - unit_rows * inner)).astype(jnp.bfloat16)
    new_gate_sum = gate_sum + jnp.dot(early_normed.T, grad_gate_in, preferred_element_type=jnp.float32)
    new_up_sum = up_sum + jnp.dot(early_normed.T, grad_up_in, preferred_element_type=jnp.float32)
    new_down_sum = down_sum + 0.5 * jnp.dot(hidden.T, grad_out, preferred_element_type=jnp.float32)
    return (out_late, grad_in, new_gate_sum, new_up_sum, new_down_sum)
```

```python
import jax
import jax.numpy as jnp
from jax import lax
from jax.sharding import PartitionSpec as P


epsilon = 1e-06
NY, NZ = 8, 8
PLANE = ("rep", "fs")


def plane_index(z, y):
    return (z % NZ) * NY + y % NY


def from_y(value, shift):
    pairs = [(plane_index(z, y), plane_index(z, y + shift)) for z in range(NZ) for y in range(NY)]
    return lax.ppermute(value, PLANE, pairs)


def from_z(value, shift):
    pairs = [(plane_index(z, y), plane_index(z + shift, y)) for z in range(NZ) for y in range(NY)]
    return lax.ppermute(value, PLANE, pairs)


def y_groups():
    return [[z * NY + y for y in range(NY)] for z in range(4)]


def at(stack, index):
    return lax.dynamic_index_in_dim(stack, index, axis=0, keepdims=False)


def contract_rows(left, right):
    return lax.dot_general(
        left, right, (((0,), (0,)), ((), ())), preferred_element_type=jnp.float32
    )


def contract_cols(left, right):
    return lax.dot_general(
        left, right, (((1,), (1,)), ((), ())), preferred_element_type=jnp.float32
    )


def whole_weights(own, z, y):
    half = len(own) // 2
    two_away = jnp.concatenate([from_z(own[:half], 2), from_z(own[half:], -2)], axis=0)
    around = jnp.stack([own, from_z(own, -1), two_away, from_z(own, 1)])
    column = lax.dynamic_slice_in_dim(jnp.concatenate([around, around]), (4 - z) % 4, 4, axis=0)
    shape = (4, NY, *own.shape)
    whole = jnp.zeros(shape, own.dtype)

    def placed(whole, piece, offset, first):
        return lax.dynamic_update_slice(whole, piece[:, None], (0, (y + offset) % NY, first, 0))

    whole = placed(whole, column, 0, 0)
    up = down = column
    for step in range(1, 4):
        up, down = from_y(up, 1), from_y(down, -1)
        whole = placed(whole, up, -step, 0)
        whole = placed(whole, down, step, 0)
    whole = placed(whole, from_y(up[:, :half], 1), 4, 0)
    whole = placed(whole, from_y(down[:, half:], -1), 4, half)
    return whole.reshape(-1, own.shape[1])


def shards(x_early, x_late, grad_out, w_gate, w_up, w_down, gate_sum, up_sum, down_sum):
    z = lax.axis_index("fs") // NY
    y = lax.axis_index("fs") % NY
    rows, width = x_early.shape
    hidden_units = w_gate.shape[1]
    weights = whole_weights(jnp.concatenate([w_gate, w_up, w_down.T], axis=1), z, y)
    gate_up = weights[:, : 2 * hidden_units]
    down_t = weights[:, 2 * hidden_units :]

    stacked = jnp.concatenate([x_early, x_late], axis=0).astype(jnp.float32)
    row_scale = lax.rsqrt(jnp.mean(stacked * stacked, axis=-1, keepdims=True) + epsilon)
    normed = (stacked * row_scale).astype(jnp.bfloat16)

    quarters = jnp.concatenate(
        [t.reshape(rows, 4, width // 4) for t in (normed[:rows], grad_out)], axis=2
    ).transpose(1, 0, 2)
    window = [
        at(quarters, z),
        from_z(at(quarters, (z + 1) % 4), 1),
        from_z(at(quarters, (z + 3) % 4), -1),
        from_z(at(quarters, (z + 2) % 4), -2),
    ]

    pre = jnp.dot(normed, gate_up, preferred_element_type=jnp.float32)
    gate_pre, up_pre = pre[:, :hidden_units], pre[:, hidden_units:]
    gate_sig = jax.nn.sigmoid(gate_pre)
    hidden = (gate_pre * gate_sig * up_pre).astype(jnp.bfloat16)
    early_gate, early_upper, early_sig = gate_pre[:rows], up_pre[:rows], gate_sig[:rows]
    grad_hidden = 0.5 * jnp.dot(grad_out, down_t, preferred_element_type=jnp.float32)
    grad_gate_in = (
        grad_hidden * early_upper * early_sig * (1.0 + early_gate * (1.0 - early_sig))
    ).astype(jnp.bfloat16)
    grad_up_in = (grad_hidden * early_gate * early_sig).astype(jnp.bfloat16)
    piece = jnp.concatenate([grad_gate_in, grad_up_in, hidden[:rows]], axis=1)
    pieces = [piece, from_z(piece, 1), from_z(piece, -1), from_z(piece, -2)]

    n_tp = lax.axis_size("tp")
    share = -(-rows // n_tp // 8) * 8
    spare = [(0, share * n_tp - rows), (0, 0)]

    def summed_rows(left, right):
        part = contract_cols(jnp.pad(left, spare), right).astype(jnp.bfloat16)
        part = part.reshape(n_tp, share, width)
        parts = lax.all_to_all(part, "tp", split_axis=0, concat_axis=0, tiled=True)
        return parts.astype(jnp.float32).sum(axis=0)

    def own_rows(value):
        padded = jnp.pad(value, spare).reshape(n_tp, share, -1)
        return at(padded, lax.axis_index("tp"))

    branch = summed_rows(hidden[rows:], down_t)
    out_late = (own_rows(x_late).astype(jnp.float32) + 0.5 * branch).astype(jnp.bfloat16)
    grad_normed = summed_rows(piece[:, : 2 * hidden_units], gate_up)
    early_scale = own_rows(row_scale[:rows])
    unit_rows = own_rows(x_early).astype(jnp.float32) * early_scale
    inner = jnp.mean(grad_normed * unit_rows, axis=-1, keepdims=True)
    grad_in = (
        own_rows(grad_out).astype(jnp.float32) + early_scale * (grad_normed - unit_rows * inner)
    ).astype(jnp.bfloat16)
    out_late = lax.all_gather(out_late, "tp", tiled=True)[:rows]
    grad_in = lax.all_gather(grad_in, "tp", tiled=True)[:rows]

    tokens = jnp.concatenate(window, axis=0)
    grads = jnp.concatenate(pieces, axis=0)
    delta = jnp.concatenate(
        [
            contract_rows(tokens[:, : width // 4], grads[:, : 2 * hidden_units]),
            0.5 * contract_rows(tokens[:, width // 4 :], grads[:, 2 * hidden_units :]),
        ],
        axis=1,
    ).astype(jnp.bfloat16)
    delta = delta.reshape(NY, -1, delta.shape[1])
    delta = lax.all_to_all(
        delta, "fs", split_axis=0, concat_axis=0, axis_index_groups=y_groups(), tiled=True
    )
    delta = delta.astype(jnp.float32).sum(axis=0).astype(jnp.bfloat16)
    other = lax.ppermute(delta, "rep", [(0, 1), (1, 0)])
    delta = delta.astype(jnp.float32) + other.astype(jnp.float32)
    return (
        out_late,
        grad_in,
        gate_sum + delta[:, :hidden_units],
        up_sum + delta[:, hidden_units : 2 * hidden_units],
        down_sum + delta[:, 2 * hidden_units :].T,
    )


def solution(mesh):
    rows = P(("rep", "fs"), None)
    up, down = P("fs", "tp"), P("tp", "fs")
    return jax.shard_map(
        shards,
        mesh=mesh,
        in_specs=(rows, rows, rows, up, up, down, up, up, down),
        out_specs=(rows, rows, up, up, down),
        check_vma=False,
    )
```

```python
import jax
import jax.numpy as jnp
from jax import lax
from jax.sharding import PartitionSpec as P


epsilon = 1e-06
NY, NZ, NX = 8, 8, 4
PLANE = ("rep", "fs")


def plane_index(z, y):
    return (z % NZ) * NY + y % NY


def sent(value, target):
    pairs = [(plane_index(z, y), plane_index(*target(z, y))) for z in range(NZ) for y in range(NY)]
    return lax.ppermute(value, PLANE, pairs)


def from_y(value, shift):
    return sent(value, lambda z, y: (z, y + shift))


def from_z(value, shift):
    return sent(value, lambda z, y: (z + shift, y))


def from_partner(value):
    return sent(value, lambda z, y: (z ^ 1, y))


def from_other_core(value):
    return lax.ppermute(value, "tp", [(t, t ^ 1) for t in range(2 * NX)])


ADDER = {0: (0, 4, 2, 6), 1: (5, 1, 7, 3)}
QUARTER = {z: q for chips in ADDER.values() for q, z in enumerate(chips)}


def to_near_owner(value):
    return sent(value, lambda z, y: (QUARTER[z] + 4 * (z // 4), y))


def to_far_owner(value):
    return sent(value, lambda z, y: (QUARTER[z] + 4 * (1 - z // 4), y))


def at(stack, index, axis=0):
    return lax.dynamic_index_in_dim(stack, index, axis=axis, keepdims=False)


def put(stack, piece, index):
    return lax.dynamic_update_index_in_dim(stack, piece, index, axis=0)


def contract_rows(left, right):
    return lax.dot_general(
        left, right, (((0,), (0,)), ((), ())), preferred_element_type=jnp.float32
    )


def contract_cols(left, right):
    return lax.dot_general(
        left, right, (((1,), (1,)), ((), ())), preferred_element_type=jnp.float32
    )


def wide(value):
    return value.astype(jnp.float32)


def narrow(value):
    return value.astype(jnp.bfloat16)


def whole_weights(mine, theirs, z, y):
    column = jnp.zeros((4, *mine.shape), mine.dtype)
    column = put(column, mine, z)
    column = put(column, from_z(theirs, 1), (z + 3) % 4)
    column = put(column, from_z(theirs, -1), (z + 1) % 4)
    column = put(column, from_z(mine, 2), (z + 2) % 4)
    half = len(mine) // 2
    whole = jnp.zeros((4, NY, *mine.shape), mine.dtype)

    def placed(whole, piece, offset, first):
        return lax.dynamic_update_slice(whole, piece[:, None], (0, (y + offset) % NY, first, 0))

    whole = placed(whole, column, 0, 0)
    up = down = column
    for step in range(1, 4):
        up, down = from_y(up, 1), from_y(down, -1)
        whole = placed(whole, up, -step, 0)
        whole = placed(whole, down, step, 0)
    whole = placed(whole, from_y(up[:, :half], 1), 4, 0)
    whole = placed(whole, from_y(down[:, half:], -1), 4, half)
    return whole.reshape(-1, mine.shape[1])


def summed_along_y(parts, y):
    def block(offset):
        return at(parts, (y + offset) % NY, axis=1)

    half = parts.shape[2] // 2
    far = block(4)
    up, down = from_y(far[:, :half], 1), from_y(far[:, half:], -1)
    none = [(0, 0), (0, half), (0, 0)], [(0, 0), (half, 0), (0, 0)]
    up, down = jnp.pad(up, none[0]), jnp.pad(down, none[1])
    for step in range(3, 0, -1):
        up = from_y(narrow(wide(block(step)) + wide(up)), 1)
        down = from_y(narrow(wide(block(-step)) + wide(down)), -1)
    return wide(block(0)) + wide(up) + wide(down)


def shards(x_early, x_late, grad_out, w_gate, w_up, w_down, gate_sum, up_sum, down_sum):
    z, y = lax.axis_index("fs") // NY, lax.axis_index("fs") % NY
    x, core = lax.axis_index("tp") // 2, lax.axis_index("tp") % 2
    parity = z % 2
    rows, width = x_early.shape
    units = w_gate.shape[1] // 2

    halves = jnp.stack(
        [
            jnp.concatenate([t[:, h * units : (h + 1) * units] for t in (w_gate, w_up, w_down.T)], axis=1)
            for h in range(2)
        ]
    )
    weights = whole_weights(at(halves, parity), at(halves, 1 - parity), z, y)
    gate_up, down_t = weights[:, : 2 * units], weights[:, 2 * units :]

    stacked = wide(jnp.stack([x_early, x_late]))
    row_scale = lax.rsqrt(jnp.mean(stacked * stacked, axis=-1, keepdims=True) + epsilon)
    normed = narrow(stacked * row_scale)

    own = jnp.stack([normed[0], normed[1], grad_out]).reshape(3, 2, rows // 2, width)
    own = [at(own, core, axis=1), at(own, 1 - core, axis=1)]
    partner = [from_partner(own[0])]
    partner.append(from_other_core(partner[0]))
    tokens = jnp.stack([jnp.stack(pair, axis=1) for pair in zip(own, partner)], axis=1)
    n_tokens = 2 * rows
    tokens = tokens.reshape(3, n_tokens, width)

    pre = jnp.dot(
        tokens[:2].reshape(2 * n_tokens, width), gate_up, preferred_element_type=jnp.float32
    )
    gate_pre, up_pre = pre[:, :units], pre[:, units:]
    gate_sig = jax.nn.sigmoid(gate_pre)
    hidden = narrow(gate_pre * gate_sig * up_pre)
    early_gate, early_upper, early_sig = gate_pre[:n_tokens], up_pre[:n_tokens], gate_sig[:n_tokens]
    grad_hidden = 0.5 * jnp.dot(tokens[2], down_t, preferred_element_type=jnp.float32)
    grad_gate_in = narrow(
        grad_hidden * early_upper * early_sig * (1.0 + early_gate * (1.0 - early_sig))
    )
    grad_up_in = narrow(grad_hidden * early_gate * early_sig)
    grads = jnp.concatenate([grad_gate_in, grad_up_in], axis=1)

    delta = jnp.concatenate(
        [contract_rows(tokens[0], grads), 0.5 * contract_rows(tokens[2], hidden[:n_tokens])], axis=1
    )
    delta = narrow(delta).reshape(4, NY, -1, 3 * units)
    delta = narrow(summed_along_y(delta, y))
    groups = [[plane_index(chip, yy) for chip in ADDER[p]] for p in ADDER for yy in range(NY)]
    delta = lax.all_to_all(delta, PLANE, 0, 0, axis_index_groups=groups, tiled=True)
    delta = narrow(wide(delta).sum(axis=0))

    share = 16
    spare = [(0, 0), (0, 0), (0, NX * share - rows // 2), (0, 0)]

    def by_share(value):
        value = jnp.pad(value.reshape(2, 2, rows // 2, -1), spare)
        return value.reshape(2, 2, NX, share, -1)

    left = jnp.stack(
        [
            by_share(jnp.pad(grads, [(0, 0), (0, units)])),
            by_share(jnp.pad(hidden[n_tokens:], [(0, 0), (2 * units, 0)])),
        ],
        axis=3,
    )
    part = narrow(contract_cols(left.reshape(-1, 3 * units), weights))
    part = part.reshape(2, 2, NX, 2 * share, width)
    part = wide(part[0]) + wide(from_other_core(part[1]))
    part = part[0] + wide(from_partner(narrow(part[1])))
    groups = [[2 * xx + c for xx in range(NX)] for c in range(2)]
    part = lax.all_to_all(narrow(part), "tp", 0, 0, axis_index_groups=groups, tiled=True)
    part = wide(part).sum(axis=0)
    grad_normed, branch = part[:share], part[share:]

    def own_rows(value):
        value = jnp.pad(value.reshape(2, rows // 2, -1), spare[1:])
        return at(at(value, core).reshape(NX, share, -1), x)

    out_late = narrow(wide(own_rows(x_late)) + 0.5 * branch)
    early_scale = own_rows(row_scale[0])
    unit_rows = wide(own_rows(x_early)) * early_scale
    inner = jnp.mean(grad_normed * unit_rows, axis=-1, keepdims=True)
    grad_in = narrow(
        wide(own_rows(grad_out)) + early_scale * (grad_normed - unit_rows * inner)
    )

    def all_rows(value):
        value = lax.all_gather(value, "tp").reshape(NX, 2, share, width)
        value = value.transpose(1, 0, 2, 3).reshape(2, NX * share, width)
        return value[:, : rows // 2].reshape(rows, width)

    out_late, grad_in = all_rows(out_late), all_rows(grad_in)

    near, far = to_near_owner(delta), to_far_owner(delta)
    first_is_near = (lax.axis_index("rep") == 0) == (parity == 0)
    lower, upper = jnp.where(first_is_near, near, far), jnp.where(first_is_near, far, near)
    gate_delta, up_delta, down_delta = (
        wide(jnp.concatenate([t[:, i * units : (i + 1) * units] for t in (lower, upper)], axis=1))
        for i in range(3)
    )
    return (out_late, grad_in, gate_sum + gate_delta, up_sum + up_delta, down_sum + down_delta.T)


def solution(mesh):
    rows = P(("rep", "fs"), None)
    up, down = P("fs", "tp"), P("tp", "fs")
    return jax.shard_map(
        shards,
        mesh=mesh,
        in_specs=(rows, rows, rows, up, up, down, up, up, down),
        out_specs=(rows, rows, up, up, down),
        check_vma=False,
    )
```

```python
import jax
import jax.numpy as jnp
from jax import lax
from jax.sharding import PartitionSpec as P


epsilon = 1e-06
NY, NZ, NX = 8, 8, 4
PLANE = ("rep", "fs")


def plane_index(z, y):
    return (z % NZ) * NY + y % NY


def sent(value, target):
    pairs = [(plane_index(z, y), plane_index(*target(z, y))) for z in range(NZ) for y in range(NY)]
    return lax.ppermute(value, PLANE, pairs)


def from_y(value, shift):
    return sent(value, lambda z, y: (z, y + shift))


def from_z(value, shift):
    return sent(value, lambda z, y: (z + shift, y))


def from_partner(value):
    return sent(value, lambda z, y: (z ^ 1, y))


def from_other_core(value):
    return lax.ppermute(value, "tp", [(t, t ^ 1) for t in range(2 * NX)])


def from_x(value, shift):
    return lax.ppermute(value, "tp", [(t, (t + 2 * shift) % (2 * NX)) for t in range(2 * NX)])


ADDER = {0: (0, 4, 2, 6), 1: (5, 1, 7, 3)}
QUARTER = {z: q for chips in ADDER.values() for q, z in enumerate(chips)}


def to_near_owner(value):
    return sent(value, lambda z, y: (QUARTER[z] + 4 * (z // 4), y))


def to_far_owner(value):
    return sent(value, lambda z, y: (QUARTER[z] + 4 * (1 - z // 4), y))


def at(stack, index, axis=0):
    return lax.dynamic_index_in_dim(stack, index, axis=axis, keepdims=False)


def put(stack, piece, index):
    return lax.dynamic_update_index_in_dim(stack, piece, index, axis=0)


def contract_rows(left, right):
    return lax.dot_general(
        left, right, (((0,), (0,)), ((), ())), preferred_element_type=jnp.float32
    )


def contract_cols(left, right):
    return lax.dot_general(
        left, right, (((1,), (1,)), ((), ())), preferred_element_type=jnp.float32
    )


def wide(value):
    return value.astype(jnp.float32)


def narrow(value):
    return value.astype(jnp.bfloat16)


def whole_weights(mine, theirs, z, y):
    column = jnp.zeros((4, *mine.shape), mine.dtype)
    column = put(column, mine, z)
    column = put(column, from_z(theirs, 1), (z + 3) % 4)
    column = put(column, from_z(theirs, -1), (z + 1) % 4)
    column = put(column, from_z(mine, 2), (z + 2) % 4)
    half = len(mine) // 2
    whole = jnp.zeros((4, NY, *mine.shape), mine.dtype)

    def placed(whole, piece, offset, first):
        return lax.dynamic_update_slice(whole, piece[:, None], (0, (y + offset) % NY, first, 0))

    whole = placed(whole, column, 0, 0)
    up = down = column
    for step in range(1, 4):
        up, down = from_y(up, 1), from_y(down, -1)
        whole = placed(whole, up, -step, 0)
        whole = placed(whole, down, step, 0)
    whole = placed(whole, from_y(up[:, :half], 1), 4, 0)
    whole = placed(whole, from_y(down[:, half:], -1), 4, half)
    return whole.reshape(-1, mine.shape[1])


def from_same_parity(value, z):
    half = len(value) // 2
    below, above = from_z(value, 2), from_z(value, -2)
    first, second = from_z(below[:half], 2), from_z(above[half:], -2)
    stack = jnp.zeros((4, *value.shape), value.dtype)
    pair = z // 2 + 2 * lax.axis_index("rep")
    stack = put(stack, value, pair)
    stack = put(stack, below, (pair + 3) % 4)
    stack = put(stack, above, (pair + 1) % 4)
    return put(stack, jnp.concatenate([first, second]), (pair + 2) % 4)


def shards(x_early, x_late, grad_out, w_gate, w_up, w_down, gate_sum, up_sum, down_sum):
    z, y = lax.axis_index("fs") // NY, lax.axis_index("fs") % NY
    x, core = lax.axis_index("tp") // 2, lax.axis_index("tp") % 2
    parity = z % 2
    rows, width = x_early.shape
    units = w_gate.shape[1] // 2

    halves = jnp.stack(
        [
            jnp.concatenate([t[:, h * units : (h + 1) * units] for t in (w_gate, w_up, w_down.T)], axis=1)
            for h in range(2)
        ]
    )
    weights = whole_weights(at(halves, parity), at(halves, 1 - parity), z, y)
    gate_up, down_t = weights[:, : 2 * units], weights[:, 2 * units :]

    stacked = wide(jnp.stack([x_early, x_late]))
    row_scale = lax.rsqrt(jnp.mean(stacked * stacked, axis=-1, keepdims=True) + epsilon)
    normed = narrow(stacked * row_scale)

    own = jnp.stack([normed[0], normed[1], grad_out]).reshape(3, 2, rows // 2, width)
    own = [at(own, core, axis=1), at(own, 1 - core, axis=1)]
    partner = [from_partner(own[0])]
    partner.append(from_other_core(partner[0]))
    tokens = jnp.stack([jnp.stack(pair, axis=1) for pair in zip(own, partner)], axis=1)
    n_tokens = 2 * rows

    quarters = own[0][::2].reshape(2, rows // 2, 4, width // 4).transpose(2, 0, 1, 3)
    quarters = jnp.stack([quarters[QUARTER[chip]] for chip in range(NZ)])
    groups = [[plane_index(chip, yy) for chip in range(NZ)] for yy in range(NY)]
    columns = lax.all_to_all(quarters, PLANE, 0, 0, axis_index_groups=groups, tiled=True)
    columns = [columns, from_other_core(columns)]
    columns = [t.reshape(NZ // 2, 2, 2, rows // 2, width // 4) for t in columns]
    columns = [jnp.stack([at(t, parity, axis=1), at(t, 1 - parity, axis=1)]) for t in columns]
    columns = jnp.stack(columns).transpose(3, 2, 0, 1, 4, 5).reshape(2, -1, width // 4)

    tokens = tokens.reshape(3, n_tokens, width)

    pre = jnp.dot(
        tokens[:2].reshape(2 * n_tokens, width), gate_up, preferred_element_type=jnp.float32
    )
    gate_pre, up_pre = pre[:, :units], pre[:, units:]
    gate_sig = jax.nn.sigmoid(gate_pre)
    hidden = narrow(gate_pre * gate_sig * up_pre)
    early_gate, early_upper, early_sig = gate_pre[:n_tokens], up_pre[:n_tokens], gate_sig[:n_tokens]
    grad_hidden = 0.5 * jnp.dot(tokens[2], down_t, preferred_element_type=jnp.float32)
    grad_gate_in = narrow(
        grad_hidden * early_upper * early_sig * (1.0 + early_gate * (1.0 - early_sig))
    )
    grad_up_in = narrow(grad_hidden * early_gate * early_sig)
    early = jnp.concatenate([grad_gate_in, grad_up_in], axis=1)

    grads = from_same_parity(jnp.concatenate([early, hidden[:n_tokens]], axis=1), z)
    grads = grads.reshape(-1, 3 * units)
    delta = jnp.concatenate(
        [
            contract_rows(columns[0], grads[:, : 2 * units]),
            0.5 * contract_rows(columns[1], grads[:, 2 * units :]),
        ],
        axis=1,
    )
    delta = narrow(delta).reshape(NY, -1, 3 * units)
    groups = [[zz * NY + yy for yy in range(NY)] for zz in range(4)]
    delta = lax.all_to_all(delta, "fs", 0, 0, axis_index_groups=groups, tiled=True)
    delta = narrow(wide(delta).sum(axis=0))

    share = 16
    spare = [(0, 0), (0, 0), (0, NX * share - rows // 2), (0, 0)]

    def by_share(value):
        value = jnp.pad(value.reshape(2, 2, rows // 2, -1), spare)
        return value.reshape(2, 2, NX, share, -1)

    left = jnp.stack(
        [
            by_share(jnp.pad(early, [(0, 0), (0, units)])),
            by_share(jnp.pad(hidden[n_tokens:], [(0, 0), (2 * units, 0)])),
        ],
        axis=3,
    )
    part = narrow(contract_cols(left.reshape(-1, 3 * units), weights))
    part = part.reshape(2, 2, NX, 2 * share, width)
    part = wide(part[0]) + wide(from_other_core(part[1]))
    from_pair = from_partner(narrow(part[1]))
    part = part[0] + wide(from_pair)
    share_for = [narrow(at(part, (x + shift) % NX)) for shift in range(NX)]
    others = [from_x(share_for[shift], shift) for shift in range(1, NX)]
    part = at(part, x) + wide(others[0]) + wide(others[1]) + wide(others[2])
    grad_normed, branch = part[:share], part[share:]

    def own_rows(value):
        value = jnp.pad(value.reshape(2, rows // 2, -1), spare[1:])
        return at(at(value, core).reshape(NX, share, -1), x)

    out_late = narrow(wide(own_rows(x_late)) + 0.5 * branch)
    early_scale = own_rows(row_scale[0])
    unit_rows = wide(own_rows(x_early)) * early_scale
    inner = jnp.mean(grad_normed * unit_rows, axis=-1, keepdims=True)
    grad_in = narrow(
        wide(own_rows(grad_out)) + early_scale * (grad_normed - unit_rows * inner)
    )

    own_done = jnp.stack([out_late, grad_in])
    done = put(jnp.zeros((NX, 2, share, width), jnp.bfloat16), own_done, x)
    for shift in range(1, NX):
        piece = from_x(own_done, shift)
        done = put(done, piece, (x + NX - shift) % NX)
    done = [done, from_other_core(done)]
    done = [t.reshape(NX, 2, share, width).transpose(1, 0, 2, 3) for t in done]
    done = [t.reshape(2, NX * share, width)[:, : rows // 2] for t in done]
    low, high = jnp.where(core == 0, done[0], done[1]), jnp.where(core == 0, done[1], done[0])
    out_late, grad_in = jnp.stack([low, high], axis=1).reshape(2, rows, width)

    near, far = to_near_owner(delta), to_far_owner(delta)
    first_is_near = (lax.axis_index("rep") == 0) == (parity == 0)
    lower, upper = jnp.where(first_is_near, near, far), jnp.where(first_is_near, far, near)
    gate_delta, up_delta, down_delta = (
        wide(jnp.concatenate([t[:, i * units : (i + 1) * units] for t in (lower, upper)], axis=1))
        for i in range(3)
    )
    return (out_late, grad_in, gate_sum + gate_delta, up_sum + up_delta, down_sum + down_delta.T)


def solution(mesh):
    rows = P(("rep", "fs"), None)
    up, down = P("fs", "tp"), P("tp", "fs")

    return jax.shard_map(
        shards,
        mesh=mesh,
        in_specs=(rows, rows, rows, up, up, down, up, up, down),
        out_specs=(rows, rows, up, up, down),
        check_vma=False,
    )
```
